32 devices in a mesh: kv: 16 (over z, y, core), tp: 2 (over x).
Axes of the slice: x: 2, y: 2, z: 4, core: 2. Of those that a mesh axis runs over, the one named last changes fastest.
Arguments:
- queries: bfloat16 [4096, 4, 128], P('kv', 'tp'), may hold values from -6 to 6
- keys: bfloat16 [4096, 4, 128], P('kv', 'tp'), may hold values from -6 to 6
- values: bfloat16 [4096, 4, 128], P('kv', 'tp'), may hold values from -6 to 6
- attended: bfloat16 [4096, 4, 128], P('kv', 'tp'), may hold values from -6 to 6
- out_grad: bfloat16 [4096, 4, 128], P('kv', 'tp'), may hold values from -6 to 6
- log_sum: float32 [4096, 4], P('kv', 'tp'), may hold values from 2.5 to 4.5
- picked: int32 [32, 16], P('kv'), may hold values from -1 to 127, as said below
- layer_input: bfloat16 [4096, 4096], P('kv'), may hold values from -0.03125 to 0.03125
Outputs:
- query_grad: float32 [4096, 4, 128], P('kv', 'tp')
- key_grad: float32 [4096, 4, 128], P('kv', 'tp')
- value_grad: float32 [4096, 4, 128], P('kv', 'tp')
- weight_grad: float32 [4096, 512], P('kv', 'tp')
The draws below stay inside these ranges and needn't reach their ends.
Inputs may be any that keep to these rules, and one draw needn't show every extreme that they name: Row r lists distinct key block numbers picked by query block r, followed by -1 to the end of the row; at least one entry is not -1, and at most 16 are. No picked block starts after the last position of its query block. With the span of a position being the position divided by 256 (rounded down), the span of every picked block is the query block's span or that span less 1, 2, 4, 8 and so on. The query blocks of one span pick at most 4 distinct blocks from any other single span.
All inputs are finite; a program needn't handle non-finite values.
Results may differ from the reference program's by a relative error of at most 0.004.
Values may be sent and summed in bfloat16 or wider, within the bound.
A program may use at most 64 MiB of HBM per device.

```python
import jax
import jax.numpy as jnp
from jax import lax

D = 4096
HEADS = 4
DH = 128
TOK_DEV = 256
QB = 128
KB = 32
MAXSEL = 16
PER_SPAN = 4
TOKENS = 4096
QBLOCKS = 32


def draw_picked(key, part):
    span_count = TOKENS // TOK_DEV
    span_blocks = TOK_DEV // KB
    query_count = TOK_DEV // QB
    levels = span_count.bit_length() - 1
    groups = levels + 1
    slot_total = groups * span_blocks
    allow_key = jax.random.fold_in(key, 11)
    score_key = jax.random.fold_in(key, 12)
    count_key_a = jax.random.fold_in(key, 13)
    count_key_b = jax.random.fold_in(key, 14)
    block_axis = jnp.arange(span_blocks, dtype=jnp.int32)
    allow_scores = jax.random.randint(allow_key, (span_count, groups, span_blocks), 0, 1 << 20, dtype=jnp.int32) * span_blocks + block_axis
    allow_rank = jnp.argsort(jnp.argsort(allow_scores, axis=-1), axis=-1)
    allowed = allow_rank < PER_SPAN
    span_index = jnp.arange(span_count, dtype=jnp.int32)[:, None, None, None]
    query_index = jnp.arange(query_count, dtype=jnp.int32)[None, :, None, None]
    group_index = jnp.arange(groups, dtype=jnp.int32)[None, None, :, None]
    block_index = block_axis[None, None, None, :]
    back_spans = jnp.where(group_index == 0, 0, jnp.left_shift(jnp.ones_like(group_index), jnp.maximum(group_index - 1, 0)))
    owner_span = span_index - back_spans
    own_usable = (group_index == 0) & (block_index * KB <= query_index * QB + QB - 1)
    far_usable = (group_index > 0) & (owner_span >= 0) & allowed[:, None, :, :]
    usable = own_usable | far_usable
    slot_index = group_index * span_blocks + block_index
    draw_scores = jax.random.randint(score_key, (span_count, query_count, groups, span_blocks), 0, 1 << 16, dtype=jnp.int32)
    unique = draw_scores * slot_total + slot_index
    masked = jnp.where(usable, unique, -1)
    group_best = jnp.max(masked, axis=-1, keepdims=True)
    last_query = query_index == query_count - 1
    forced = usable & (masked == group_best) | usable & last_query & (group_index == 1)
    ranked = jnp.where(usable, unique + jnp.where(forced, 1 << 28, 0), -1)
    half_most = MAXSEL // 2
    extra_picks = jax.random.randint(count_key_a, (span_count, query_count), 0, half_most + 1, dtype=jnp.int32) * jax.random.randint(count_key_b, (span_count, query_count), 0, half_most + 1, dtype=jnp.int32) // half_most
    usable_count = jnp.sum(usable.astype(jnp.int32), axis=(2, 3))
    forced_count = jnp.sum(forced.astype(jnp.int32), axis=(2, 3))
    last_row = (jnp.arange(query_count, dtype=jnp.int32) == query_count - 1)[None, :]
    wanted = jnp.where(last_row, MAXSEL, jnp.maximum(half_most + extra_picks, forced_count))
    pick_count = jnp.minimum(wanted, usable_count)
    flat_ranked = ranked.reshape(span_count, query_count, slot_total)
    top_values, top_slots = lax.top_k(flat_ranked, MAXSEL)
    chosen_group = top_slots // span_blocks
    chosen_block = top_slots % span_blocks
    chosen_back = jnp.where(chosen_group == 0, 0, jnp.left_shift(jnp.ones_like(chosen_group), jnp.maximum(chosen_group - 1, 0)))
    chosen_span = jnp.arange(span_count, dtype=jnp.int32)[:, None, None] - chosen_back
    chosen_ids = chosen_span * span_blocks + chosen_block
    position = jnp.arange(MAXSEL, dtype=jnp.int32)[None, None, :]
    chosen_ids = jnp.where(position < pick_count[:, :, None], chosen_ids, -1)
    return chosen_ids.reshape(span_count * query_count, MAXSEL).astype(jnp.int32)


def raised(array, own_key, source, target, shards_of, factor):
    def block_of(axis_at):
        return (jnp.arange(array.shape[axis_at]) // (array.shape[axis_at] // shards_of)).reshape((-1,) + (1,) * (array.ndim - 1 - axis_at))

    one_side = jax.random.permutation(own_key, shards_of)[block_of(target)]
    other_side = (block_of(target) + shards_of // 2) % shards_of
    return jnp.where((block_of(source) == one_side) | (block_of(source) == other_side), factor * array, array)


def level_of(stream_key, extent, split, smallest, high):
    gain, own = 1.0, jax.random.fold_in(stream_key, 6)
    for axis_at, blocks in split:
        draws = jnp.exp(jax.random.uniform(jax.random.fold_in(own, axis_at), (blocks,), jnp.float32, smallest / len(split), high / len(split)))
        gain = gain * jnp.repeat(draws, extent[axis_at] // blocks).reshape([-1 if axis == axis_at else 1 for axis in range(len(extent))])
    return gain


def gaussian(rng, dims, scale, bound, split=(), kind=jnp.bfloat16):
    entries = scale * jax.random.normal(rng, dims, jnp.float32)
    if split:
        entries = entries * level_of(rng, dims, split, -0.22, 0.18)
    return jnp.clip(entries, -bound, bound).astype(kind)


def heavy_noise(key, extent, spread, bound, cuts, heavy, kind=jnp.bfloat16):
    entries = spread * jax.random.normal(key, extent, jnp.float32)
    if cuts:
        entries = entries * level_of(key, extent, cuts, -0.22, 0.18)
    return jnp.clip(raised(entries, jax.random.fold_in(key, 3), *heavy), -bound, bound).astype(kind)


def setup_inputs(seed: int = 0) -> dict:
    arg_keys = jax.random.split(jax.random.key(seed), 9)
    queries = gaussian(arg_keys[0], (TOKENS, HEADS, DH), 1.0, 6.0, ((0, 16), (1, 2)))
    keys = gaussian(arg_keys[1], (TOKENS, HEADS, DH), 1.0, 6.0, ((0, 16), (1, 2)))
    values = gaussian(arg_keys[2], (TOKENS, HEADS, DH), 1.0, 6.0, ((0, 16), (1, 2)))
    attended = gaussian(arg_keys[3], (TOKENS, HEADS, DH), 1.0, 6.0, ((0, 16), (1, 2)))
    out_grad = gaussian(arg_keys[4], (TOKENS, HEADS, DH), 1.0, 6.0, ((0, 16), (1, 2)))
    log_sum = jnp.clip(2.5 + 2.0 * jax.random.uniform(arg_keys[5], (TOKENS, HEADS), jnp.float32) ** level_of(arg_keys[5], (TOKENS, HEADS), ((0, 16), (1, 2)), -0.2, 0.2), 2.5, 4.5)
    picked = draw_picked(jax.random.fold_in(arg_keys[8], 71), 0)
    layer_input = heavy_noise(arg_keys[7], (TOKENS, D), 0.004, 0.03125, ((0, 16),), (0, 1, 16, 2.0))
    return dict(queries=queries, keys=keys, values=values, attended=attended, out_grad=out_grad, log_sum=log_sum, picked=picked, layer_input=layer_input)


def reference(queries, keys, values, attended, out_grad, log_sum, picked, layer_input):
    score_scale = DH ** -0.5
    row_dots = jnp.sum(out_grad.astype(jnp.float32) * attended.astype(jnp.float32), axis=-1)
    key_offsets = jnp.arange(KB, dtype=jnp.int32)
    query_offsets = jnp.arange(QB, dtype=jnp.int32)

    def one_block(carry, block_index):
        key_sums, value_sums = carry
        listed = picked[block_index]
        listed_live = listed >= 0
        gather_rows = (jnp.where(listed_live, listed, 0)[:, None] * KB + key_offsets[None, :]).reshape(-1).astype(jnp.int32)
        key_live = jnp.repeat(listed_live, KB)
        first_query = (block_index * QB).astype(jnp.int32)
        query_pos = first_query + query_offsets
        pair_live = key_live[None, :] & (gather_rows[None, :] <= query_pos[:, None])
        query_rows = lax.dynamic_slice_in_dim(queries, first_query, QB, 0).astype(jnp.float32)
        grad_rows = lax.dynamic_slice_in_dim(out_grad, first_query, QB, 0).astype(jnp.float32)
        stored = lax.dynamic_slice_in_dim(log_sum, first_query, QB, 0)
        block_dots = lax.dynamic_slice_in_dim(row_dots, first_query, QB, 0)
        key_rows = keys[gather_rows].astype(jnp.float32)
        value_rows = values[gather_rows].astype(jnp.float32)
        scores = jnp.einsum("qhd,khd->hqk", query_rows, key_rows) * score_scale
        weights = jnp.where(pair_live[None], jnp.exp(scores - stored.T[:, :, None]), 0.0)
        slopes = jnp.einsum("qhd,khd->hqk", grad_rows, value_rows)
        score_grad = weights * (slopes - block_dots.T[:, :, None])
        weight_pairs = lax.optimization_barrier(weights.astype(jnp.bfloat16)).astype(jnp.float32)
        grad_pairs = lax.optimization_barrier(score_grad.astype(jnp.bfloat16)).astype(jnp.float32)
        query_grad = jnp.einsum("hqk,khd->qhd", grad_pairs, key_rows) * score_scale
        key_terms = jnp.einsum("hqk,qhd->khd", grad_pairs, query_rows) * score_scale
        value_terms = jnp.einsum("hqk,qhd->khd", weight_pairs, grad_rows)
        key_sums = key_sums.at[gather_rows].add(key_terms)
        value_sums = value_sums.at[gather_rows].add(value_terms)
        return (key_sums, value_sums), query_grad

    empty = jnp.zeros(keys.shape, jnp.float32)
    (key_grad, value_grad), query_grad = lax.scan(one_block, (empty, empty), jnp.arange(QBLOCKS, dtype=jnp.int32))
    query_grad = query_grad.reshape(TOKENS, HEADS, DH)
    value_round = value_grad.astype(jnp.bfloat16).reshape(TOKENS, HEADS * DH)
    weight_grad = lax.dot_general(layer_input, value_round, (((0,), (0,)), ((), ())), preferred_element_type=jnp.float32)
    return query_grad, key_grad, value_grad, weight_grad
```

```python
import functools

import jax
import jax.numpy as jnp
from jax import lax
from jax.experimental import pallas as pl
from jax.experimental.pallas import tpu as pltpu
from jax.sharding import PartitionSpec as P

QB = 128
KB = 32
PER_SPAN = 4
COMPACT = PER_SPAN * KB
CHUNKS = 8
F32 = jnp.float32
BF16 = jnp.bfloat16


def xor(value, bits):
    out = value
    for i in range(bits.bit_length()):
        if bits >> i & 1:
            out = out + (1 << i) - (2 << i) * lax.rem(value // (1 << i), 2)
    return out


def dot_nt(a, b):
    return lax.dot_general(a, b, (((1,), (1,)), ((), ())), preferred_element_type=F32)


def dot_tn(a, b):
    return lax.dot_general(a, b, (((0,), (0,)), ((), ())), preferred_element_type=F32)


def dot_nn(a, b):
    return lax.dot_general(a, b, (((1,), (0,)), ((), ())), preferred_element_type=F32)


def body(
    n, levels, heads, dh,
    picked, q, k, v, att, og, log_sum, x_hbm,
    dq_out, dk_out, dv_out, wg_out,
    x, slot, slot_in, pick, ksend, kin, vsend, vin, dvsend, dvin, dksend, dkin,
    wts, part, got1, send2, got2, send3, got3,
    x_sem, slot_ss, slot_rs, k_ss, k_rs, v_ss, v_rs, dv_ss, dv_rs, dk_ss, dk_rs,
    s1_ss, s1_rs, s2_ss, s2_rs, s3_ss, s3_rs,
):
    me = lax.axis_index("kv")
    tok, cols = q.shape
    query_count = tok // QB
    span_blocks = tok // KB
    rows = slot.shape[0]
    scale = dh ** (-0.5)
    quarter = n // 4
    rb = wg_out.shape[0]
    order = list(reversed(range(levels)))

    def to(offset):
        return {"kv": lax.rem(me + offset + n, n)}

    def flipped(bits):
        low = lax.rem(me, 4)
        high = me // 4
        if bits == 1:
            return {"kv": me + 1 - 2 * lax.rem(me, 2)}
        if bits == 2:
            return {"kv": me + 2 - 4 * (low // 2)}
        return {"kv": xor(high, bits // 4) * 4 + low}

    def remote(src, dst, ss, rs, device):
        return pltpu.make_async_remote_copy(
            src_ref=src, dst_ref=dst, send_sem=ss, recv_sem=rs,
            device_id=device, device_id_type=pl.DeviceIdType.MESH,
        )

    load_x = pltpu.make_async_copy(x_hbm, x, x_sem)
    load_x.start()
    barrier = pltpu.get_barrier_semaphore()
    greeted = [to(1 << l) for l in range(levels)] + [to(-(1 << l)) for l in range(levels)]
    greeted += [flipped(1), flipped(2)] + [flipped(4 * b) for b in range(1, quarter)]
    for device in greeted:
        pl.semaphore_signal(
            barrier, inc=1, device_id=device, device_id_type=pl.DeviceIdType.MESH
        )

    row = lax.broadcasted_iota(jnp.int32, (rows, tok), 0)
    lane = lax.broadcasted_iota(jnp.int32, (rows, tok), 1)
    back = jnp.zeros((rows, tok), jnp.int32)
    for l in range(levels):
        back = jnp.where(row == l + 1, 1 << l, back)
    ids = jnp.where(row <= levels, (me - back) * span_blocks + lane // KB, -2)
    live = []
    for b in range(query_count):
        hit = jnp.zeros((rows, tok), jnp.int32)
        for s in range(picked.shape[1]):
            p = picked[b, s]
            hit = jnp.where(ids == jnp.where(p < 0, -(1 << 30), p), 1, hit)
        live.append(hit.astype(F32))
    need = functools.reduce(jnp.maximum, live)
    below = lax.broadcasted_iota(jnp.int32, (tok, tok), 0)
    above = lax.broadcasted_iota(jnp.int32, (tok, tok), 1)
    steps = jnp.where((below % KB == 0) & (below // KB < above // KB), 1.0, 0.0).astype(BF16)
    rank = dot_nn(need.astype(BF16), steps)
    slot[...] = jnp.where(need > 0, rank * KB + (lane % KB).astype(F32), -1.0)

    pl.semaphore_wait(barrier, len(greeted))
    slot_copies = {}
    for l in order:
        slot_copies[l] = remote(
            slot, slot_in.at[l], slot_ss.at[l], slot_rs.at[l], to(-(1 << l))
        )
        slot_copies[l].start()

    def one_hot(row_values):
        sub = lax.broadcasted_iota(jnp.int32, (COMPACT, tok), 0).astype(F32)
        return jnp.where(sub == row_values, 1.0, 0.0).astype(BF16)

    head = [slice(h * dh, (h + 1) * dh) for h in range(heads)]
    k_copies, v_copies = {}, {}
    for l in order:
        slot_copies[l].wait_recv()
        chosen = one_hot(slot_in[l, l + 1 : l + 2, :])
        pick[l] = chosen
        ksend[l] = dot_nn(chosen, k[...]).astype(BF16)
        k_copies[l] = remote(ksend.at[l], kin.at[l], k_ss.at[l], k_rs.at[l], to(1 << l))
        k_copies[l].start()
    for l in order:
        vsend[l] = dot_nn(pick[l], v[...]).astype(BF16)
        v_copies[l] = remote(vsend.at[l], vin.at[l], v_ss.at[l], v_rs.at[l], to(1 << l))
        v_copies[l].start()

    dots = [
        jnp.sum(og[:, c].astype(F32) * att[:, c].astype(F32), axis=1, keepdims=True) for c in head
    ]
    stored = [log_sum[:, h : h + 1] for h in range(heads)]

    def spread(pieces):
        return jnp.concatenate(
            [jnp.broadcast_to(p, (QB, p.shape[1])) for p in pieces], axis=0
        )

    own_live = spread([m[0:1, :] for m in live]) > 0
    own_live = own_live & (above <= below)
    for h, c in enumerate(head):
        w = jnp.where(own_live, jnp.exp(dot_nt(q[:, c], k[:, c]) * scale - stored[h]), 0.0)
        dv_out[:, c] = dot_tn(w.astype(BF16), og[:, c])
        g = (w * (dot_nt(og[:, c], v[:, c]) - dots[h])).astype(BF16)
        dq_out[:, c] = dot_nn(g, k[:, c])
        dk_out[:, c] = dot_tn(g, q[:, c])

    dv_copies, dk_copies = {}, {}
    for l in order:
        mine = one_hot(slot[l + 1 : l + 2, :])
        mask = spread([dot_nt(m.astype(BF16), mine)[l + 1 : l + 2, :] for m in live]) > 0
        k_copies[l].wait_recv()
        for h, c in enumerate(head):
            w = jnp.where(mask, jnp.exp(dot_nt(q[:, c], kin[l, :, c]) * scale - stored[h]), 0.0)
            wts[l, h] = w
            dvsend[l, :, c] = dot_tn(w.astype(BF16), og[:, c]).astype(BF16)
        dv_copies[l] = remote(
            dvsend.at[l], dvin.at[l], dv_ss.at[l], dv_rs.at[l], to(-(1 << l))
        )
        dv_copies[l].start()
    for l in order:
        v_copies[l].wait_recv()
        for h, c in enumerate(head):
            g = (wts[l, h] * (dot_nt(og[:, c], vin[l, :, c]) - dots[h])).astype(BF16)
            dq_out[:, c] += dot_nn(g, kin[l, :, c])
            dksend[l, :, c] = (dot_tn(g, q[:, c]) * scale).astype(BF16)
        dk_copies[l] = remote(
            dksend.at[l], dkin.at[l], dk_ss.at[l], dk_rs.at[l], to(-(1 << l))
        )
        dk_copies[l].start()
    dq_out[...] = dq_out[...] * scale

    total = dv_out[...]
    for l in order:
        dv_copies[l].wait_recv()
        total += dot_tn(pick[l], dvin[l])
    dv_out[...] = total
    rounded = total.astype(BF16)
    load_x.wait()
    core = lax.rem(me, 2)
    per = (n // 2) // CHUNKS
    width = x.shape[1] // CHUNKS
    s1 = []
    for i in range(CHUNKS):
        w = dot_tn(x[:, i * width : (i + 1) * width], rounded).reshape(per, 2, rb, cols)
        part[0, i * per : (i + 1) * per] = w[:, 0]
        part[1, i * per : (i + 1) * per] = w[:, 1]
        copy = remote(
            part.at[1 - core, pl.ds(i * per, per)], got1.at[pl.ds(i * per, per)],
            s1_ss.at[i], s1_rs.at[i], flipped(1),
        )
        copy.start()
        s1.append(copy)
    for copy in s1:
        copy.wait()
    up = lax.rem(me, 4) // 2
    high = me // 4
    s2, s3 = [], []
    for b in reversed(range(quarter)):
        at = 2 * xor(high, b) + 1 - up
        send2[b] = (part[core, at] + got1[at]).astype(BF16)
        copy = remote(send2.at[b], got2.at[b], s2_ss.at[b], s2_rs.at[b], flipped(2))
        copy.start()
        s2.append(copy)
    for b, copy in zip(reversed(range(quarter)), s2):
        at = 2 * xor(high, b) + up
        kept = part[core, at] + got1[at]
        copy.wait_recv()
        kept = kept + got2[b].astype(F32)
        if b == 0:
            wg_out[...] = kept
        else:
            send3[b] = kept.astype(BF16)
            copy = remote(send3.at[b], got3.at[b], s3_ss.at[b], s3_rs.at[b], flipped(4 * b))
            copy.start()
            s3.append(copy)

    total = dk_out[...] * scale
    for l in order:
        dk_copies[l].wait_recv()
        total += dot_tn(pick[l], dkin[l])
    dk_out[...] = total

    for b, copy in zip(reversed(range(1, quarter)), s3):
        copy.wait_recv()
        wg_out[...] += got3[b].astype(F32)
    for copies in (slot_copies, k_copies, v_copies, dv_copies, dk_copies):
        for l in order:
            copies[l].wait_send()
    for copy in s2 + s3:
        copy.wait_send()


def per_device(queries, keys, values, attended, out_grad, log_sum, picked, layer_input):
    tok, heads, dh = queries.shape
    n = lax.axis_size("kv")
    levels = n.bit_length() - 1
    cols = heads * dh
    width = layer_input.shape[1]
    rb = width // n
    rows = (levels + 1 + 7) // 8 * 8
    flat = [a.reshape(tok, cols) for a in (queries, keys, values, attended, out_grad)]
    vmem = pl.BlockSpec(memory_space=pltpu.VMEM)
    sems = pltpu.SemaphoreType.DMA
    level_buf = pltpu.VMEM((levels, COMPACT, cols), BF16)
    out = pl.pallas_call(
        functools.partial(body, n, levels, heads, dh),
        out_shape=[jax.ShapeDtypeStruct((tok, cols), F32)] * 3
        + [jax.ShapeDtypeStruct((rb, cols), F32)],
        in_specs=[pl.BlockSpec(memory_space=pltpu.SMEM)] + [vmem] * 6
        + [pl.BlockSpec(memory_space=pl.ANY)],
        out_specs=[vmem] * 4,
        scratch_shapes=[
            pltpu.VMEM((tok, width), BF16),
            pltpu.VMEM((rows, tok), F32),
            pltpu.VMEM((levels, rows, tok), F32),
            pltpu.VMEM((levels, COMPACT, tok), BF16),
        ]
        + [level_buf] * 8
        + [
            pltpu.VMEM((levels, heads, tok, COMPACT), F32),
            pltpu.VMEM((2, n // 2, rb, cols), F32),
            pltpu.VMEM((n // 2, rb, cols), F32),
            pltpu.VMEM((n // 4, rb, cols), BF16),
            pltpu.VMEM((n // 4, rb, cols), BF16),
            pltpu.VMEM((n // 4, rb, cols), BF16),
            pltpu.VMEM((n // 4, rb, cols), BF16),
            sems,
        ]
        + [sems((levels,))] * 10
        + [sems((CHUNKS,))] * 2
        + [sems((n // 4,))] * 4,
        compiler_params=pltpu.CompilerParams(
            collective_id=0, has_side_effects=True, vmem_limit_bytes=48 * 1024 * 1024
        ),
    )(picked, *flat, log_sum, layer_input)
    grads = [g.reshape(tok, heads, dh) for g in out[:3]]
    return (*grads, out[3])


def solution(mesh):
    placed = (P("kv", "tp", None),) * 5 + (P("kv", "tp"), P("kv", None), P("kv", None))
    return jax.shard_map(
        per_device,
        mesh=mesh,
        in_specs=placed,
        out_specs=(P("kv", "tp", None), P("kv", "tp", None), P("kv", "tp", None), P("kv", "tp")),
        check_vma=False,
    )
```

```python
import functools

import jax
import jax.numpy as jnp
from jax import lax
from jax.experimental import pallas as pl
from jax.experimental.pallas import tpu as pltpu
from jax.sharding import PartitionSpec as P

QB = 128
KB = 32
PER_SPAN = 4
COMPACT = PER_SPAN * KB
CHUNKS = 8
F32 = jnp.float32
BF16 = jnp.bfloat16


def xor(value, bits):
    out = value
    for i in range(bits.bit_length()):
        if bits >> i & 1:
            out = out + (1 << i) - (2 << i) * lax.rem(value // (1 << i), 2)
    return out


def dot_nt(a, b):
    return lax.dot_general(a, b, (((1,), (1,)), ((), ())), preferred_element_type=F32)


def dot_tn(a, b):
    return lax.dot_general(a, b, (((0,), (0,)), ((), ())), preferred_element_type=F32)


def dot_nn(a, b):
    return lax.dot_general(a, b, (((1,), (0,)), ((), ())), preferred_element_type=F32)


def body(
    n, levels, heads, dh,
    picked_hbm, q_hbm, k_hbm, v_hbm, att_hbm, og_hbm, log_sum, x_hbm,
    dq_out, dk_out, dv_out, wg_out,
    picked, raw, q, k, v, att, og, x, xt, slot, slot_in, pick, ksend, kin, vsend, vin, dvsend, dvin, dksend, dkin,
    wts, part, got1, send2, got2, send3, got3,
    x_sem, picked_sem, raw_sem, slot_ss, slot_rs, k_ss, k_rs, v_ss, v_rs, dv_ss, dv_rs, dk_ss, dk_rs,
    s1_ss, s1_rs, s2_ss, s2_rs, s3_ss, s3_rs,
):
    me = lax.axis_index("kv")
    tok, cols = q.shape
    query_count = tok // QB
    span_blocks = tok // KB
    rows = slot.shape[0]
    scale = dh ** (-0.5)
    quarter = n // 4
    rb = wg_out.shape[0]
    order = list(reversed(range(levels)))

    def to(offset):
        return {"kv": lax.rem(me + offset + n, n)}

    def flipped(bits):
        low = lax.rem(me, 4)
        high = me // 4
        if bits == 1:
            return {"kv": me + 1 - 2 * lax.rem(me, 2)}
        if bits == 2:
            return {"kv": me + 2 - 4 * (low // 2)}
        return {"kv": xor(high, bits // 4) * 4 + low}

    def remote(src, dst, ss, rs, device):
        return pltpu.make_async_remote_copy(
            src_ref=src, dst_ref=dst, send_sem=ss, recv_sem=rs,
            device_id=device, device_id_type=pl.DeviceIdType.MESH,
        )

    load_picked = pltpu.make_async_copy(picked_hbm, picked, picked_sem)
    load_picked.start()
    loads = {}
    for i, (src, dst) in enumerate(
        ((k_hbm, k), (v_hbm, v), (q_hbm, q), (og_hbm, og), (att_hbm, att))
    ):
        loads[i] = (pltpu.make_async_copy(src, raw.at[i], raw_sem.at[i]), dst)
        loads[i][0].start()

    def settle(i):
        copy, dst = loads[i]
        copy.wait()
        for h in range(heads):
            dst[:, h * dh : (h + 1) * dh] = raw[i, :, h, :]

    load_x = pltpu.make_async_copy(x_hbm, x, x_sem)
    load_x.start()
    barrier = pltpu.get_barrier_semaphore()
    greeted = [to(1 << l) for l in range(levels)] + [to(-(1 << l)) for l in range(levels)]
    greeted += [flipped(1), flipped(2)] + [flipped(4 * b) for b in range(1, quarter)]
    for device in greeted:
        pl.semaphore_signal(
            barrier, inc=1, device_id=device, device_id_type=pl.DeviceIdType.MESH
        )

    row = lax.broadcasted_iota(jnp.int32, (rows, tok), 0)
    lane = lax.broadcasted_iota(jnp.int32, (rows, tok), 1)
    back = jnp.zeros((rows, tok), jnp.int32)
    for l in range(levels):
        back = jnp.where(row == l + 1, 1 << l, back)
    ids = jnp.where(row <= levels, (me - back) * span_blocks + lane // KB, -2)
    load_picked.wait()
    live = []
    for b in range(query_count):
        hit = jnp.zeros((rows, tok), jnp.int32)
        for s in range(picked.shape[1]):
            p = picked[b, s]
            hit = jnp.where(ids == jnp.where(p < 0, -(1 << 30), p), 1, hit)
        live.append(hit.astype(F32))
    need = functools.reduce(jnp.maximum, live)
    below = lax.broadcasted_iota(jnp.int32, (tok, tok), 0)
    above = lax.broadcasted_iota(jnp.int32, (tok, tok), 1)
    steps = jnp.where((below % KB == 0) & (below // KB < above // KB), 1.0, 0.0).astype(BF16)
    rank = dot_nn(need.astype(BF16), steps)
    slot[...] = jnp.where(need > 0, rank * KB + (lane % KB).astype(F32), -1.0)

    settle(0)
    settle(1)
    pl.semaphore_wait(barrier, len(greeted))

    def sends_up(l):
        return me + (1 << l) < n

    def sends_down(l):
        return me >= 1 << l

    slot_copies = {}
    for l in order:
        slot_copies[l] = remote(
            slot, slot_in.at[l], slot_ss.at[l], slot_rs.at[l], to(-(1 << l))
        )
        pl.when(sends_down(l))(slot_copies[l].start)

    def one_hot(row_values):
        sub = lax.broadcasted_iota(jnp.int32, (COMPACT, tok), 0).astype(F32)
        return jnp.where(sub == row_values, 1.0, 0.0).astype(BF16)

    head = [slice(h * dh, (h + 1) * dh) for h in range(heads)]
    k_copies, v_copies, dv_copies, dk_copies = {}, {}, {}, {}
    for l in order:
        k_copies[l] = remote(ksend.at[l], kin.at[l], k_ss.at[l], k_rs.at[l], to(1 << l))
        v_copies[l] = remote(vsend.at[l], vin.at[l], v_ss.at[l], v_rs.at[l], to(1 << l))
        dv_copies[l] = remote(
            dvsend.at[l], dvin.at[l], dv_ss.at[l], dv_rs.at[l], to(-(1 << l))
        )
        dk_copies[l] = remote(
            dksend.at[l], dkin.at[l], dk_ss.at[l], dk_rs.at[l], to(-(1 << l))
        )
    for l in order:

        @pl.when(sends_up(l))
        def _(l=l):
            slot_copies[l].wait_recv()
            chosen = one_hot(slot_in[l, l + 1 : l + 2, :])
            pick[l] = chosen
            ksend[l] = dot_nn(chosen, k[...]).astype(BF16)
            k_copies[l].start()

    for l in order:

        @pl.when(sends_up(l))
        def _(l=l):
            vsend[l] = dot_nn(pick[l], v[...]).astype(BF16)
            v_copies[l].start()

    for i in range(2, 5):
        settle(i)
    dots = []
    for c in head:
        column = jnp.sum(og[:, c].astype(F32) * att[:, c].astype(F32), axis=1, keepdims=True)
        dots.append(jnp.transpose(jnp.broadcast_to(column, (tok, 128)))[0:1, :])
    stored = [log_sum[h : h + 1, :] for h in range(heads)]

    def key_mask(chosen, r):
        pieces = []
        for m in live:
            column = dot_nt(chosen, m.astype(BF16))[:, r : r + 1]
            pieces.append(jnp.broadcast_to(column, (column.shape[0], QB)))
        return jnp.concatenate(pieces, axis=1) > 0

    own_mask = key_mask(jnp.where(below == above, 1.0, 0.0).astype(BF16), 0) & (below <= above)
    for h, c in enumerate(head):
        w = jnp.where(own_mask, jnp.exp(dot_nt(k[:, c], q[:, c]) * scale - stored[h]), 0.0)
        dv_out[:, c] = dot_nn(w.astype(BF16), og[:, c])
        g = (w * (dot_nt(v[:, c], og[:, c]) - dots[h])).astype(BF16)
        dk_out[:, c] = dot_nn(g, q[:, c])
        dq_out[:, c] = dot_tn(g, k[:, c])

    masks = {
        l: key_mask(one_hot(slot[l + 1 : l + 2, :]), l + 1) for l in order
    }
    load_x.wait()
    width = x.shape[1] // CHUNKS
    for i in range(CHUNKS):
        xt[i * width : (i + 1) * width, :] = jnp.transpose(x[:, i * width : (i + 1) * width])
    for l in order:

        @pl.when(sends_down(l))
        def _(l=l):
            k_copies[l].wait_recv()
            for h, c in enumerate(head):
                w = jnp.where(
                    masks[l], jnp.exp(dot_nt(kin[l, :, c], q[:, c]) * scale - stored[h]), 0.0
                )
                wts[l, h] = w
                dvsend[l, :, c] = dot_nn(w.astype(BF16), og[:, c]).astype(BF16)
            dv_copies[l].start()

    for l in order:

        @pl.when(sends_down(l))
        def _(l=l):
            v_copies[l].wait_recv()
            for h, c in enumerate(head):
                g = (wts[l, h] * (dot_nt(vin[l, :, c], og[:, c]) - dots[h])).astype(BF16)
                dksend[l, :, c] = (dot_nn(g, q[:, c]) * scale).astype(BF16)
                dq_out[:, c] += dot_tn(g, kin[l, :, c])
            dk_copies[l].start()

    dq_out[...] = dq_out[...] * scale

    for l in order:

        @pl.when(sends_up(l))
        def _(l=l):
            dv_copies[l].wait_recv()
            dv_out[...] += dot_tn(pick[l], dvin[l])

    rounded = dv_out[...].astype(BF16)
    core = lax.rem(me, 2)
    per = (n // 2) // CHUNKS
    s1 = []
    for i in range(CHUNKS):
        w = dot_nn(xt[i * width : (i + 1) * width, :], rounded).reshape(per, 2, rb, cols)
        part[0, i * per : (i + 1) * per] = w[:, 0]
        part[1, i * per : (i + 1) * per] = w[:, 1]
        copy = remote(
            part.at[1 - core, pl.ds(i * per, per)], got1.at[pl.ds(i * per, per)],
            s1_ss.at[i], s1_rs.at[i], flipped(1),
        )
        copy.start()
        s1.append(copy)
    for copy in s1:
        copy.wait()
    up = lax.rem(me, 4) // 2
    high = me // 4
    s2, s3 = [], []
    for b in reversed(range(quarter)):
        at = 2 * xor(high, b) + 1 - up
        send2[b] = (part[core, at] + got1[at]).astype(BF16)
        copy = remote(send2.at[b], got2.at[b], s2_ss.at[b], s2_rs.at[b], flipped(2))
        copy.start()
        s2.append(copy)
    for b, copy in zip(reversed(range(quarter)), s2):
        at = 2 * xor(high, b) + up
        kept = part[core, at] + got1[at]
        copy.wait_recv()
        kept = kept + got2[b].astype(F32)
        if b == 0:
            wg_out[...] = kept
        else:
            send3[b] = kept.astype(BF16)
            copy = remote(send3.at[b], got3.at[b], s3_ss.at[b], s3_rs.at[b], flipped(4 * b))
            copy.start()
            s3.append(copy)

    dk_out[...] = dk_out[...] * scale
    for l in order:

        @pl.when(sends_up(l))
        def _(l=l):
            dk_copies[l].wait_recv()
            dk_out[...] += dot_tn(pick[l], dkin[l])

    for b, copy in zip(reversed(range(1, quarter)), s3):
        copy.wait_recv()
        wg_out[...] += got3[b].astype(F32)
    for l in order:
        for copies in (slot_copies, dv_copies, dk_copies):
            pl.when(sends_down(l))(copies[l].wait_send)
        for copies in (k_copies, v_copies):
            pl.when(sends_up(l))(copies[l].wait_send)
    for copy in s2 + s3:
        copy.wait_send()


def per_device(queries, keys, values, attended, out_grad, log_sum, picked, layer_input):
    tok, heads, dh = queries.shape
    n = lax.axis_size("kv")
    levels = n.bit_length() - 1
    cols = heads * dh
    width = layer_input.shape[1]
    rb = width // n
    rows = (levels + 1 + 7) // 8 * 8
    hbm = pl.BlockSpec(memory_space=pltpu.HBM)
    vmem = pl.BlockSpec(memory_space=pltpu.VMEM)
    sems = pltpu.SemaphoreType.DMA
    level_buf = pltpu.VMEM((levels, COMPACT, cols), BF16)
    out = pl.pallas_call(
        functools.partial(body, n, levels, heads, dh),
        out_shape=[jax.ShapeDtypeStruct((tok, cols), F32)] * 3
        + [jax.ShapeDtypeStruct((rb, cols), F32)],
        in_specs=[hbm] * 6 + [vmem, hbm],
        out_specs=[vmem] * 4,
        scratch_shapes=[
            pltpu.SMEM(picked.shape, jnp.int32),
            pltpu.VMEM((5, tok, heads, dh), BF16),
        ]
        + [pltpu.VMEM((tok, cols), BF16)] * 5
        + [
            pltpu.VMEM((tok, width), BF16),
            pltpu.VMEM((width, tok), BF16),
            pltpu.VMEM((rows, tok), F32),
            pltpu.VMEM((levels, rows, tok), F32),
            pltpu.VMEM((levels, COMPACT, tok), BF16),
        ]
        + [level_buf] * 8
        + [
            pltpu.VMEM((levels, heads, COMPACT, tok), F32),
            pltpu.VMEM((2, n // 2, rb, cols), F32),
            pltpu.VMEM((n // 2, rb, cols), F32),
            pltpu.VMEM((n // 4, rb, cols), BF16),
            pltpu.VMEM((n // 4, rb, cols), BF16),
            pltpu.VMEM((n // 4, rb, cols), BF16),
            pltpu.VMEM((n // 4, rb, cols), BF16),
            sems,
            sems,
            sems((5,)),
        ]
        + [sems((levels,))] * 10
        + [sems((CHUNKS,))] * 2
        + [sems((n // 4,))] * 4,
        compiler_params=pltpu.CompilerParams(
            collective_id=0, has_side_effects=True, vmem_limit_bytes=48 * 1024 * 1024
        ),
    )(picked, queries, keys, values, attended, out_grad, log_sum.T, layer_input)
    grads = [g.reshape(tok, heads, dh) for g in out[:3]]
    return (*grads, out[3])


def solution(mesh):
    placed = (P("kv", "tp", None),) * 5 + (P("kv", "tp"), P("kv", None), P("kv", None))
    return jax.shard_map(
        per_device,
        mesh=mesh,
        in_specs=placed,
        out_specs=(P("kv", "tp", None), P("kv", "tp", None), P("kv", "tp", None), P("kv", "tp")),
        check_vma=False,
    )
```

```python
import functools

import jax
import jax.numpy as jnp
from jax import lax
from jax.experimental import pallas as pl
from jax.experimental.pallas import tpu as pltpu
from jax.sharding import PartitionSpec as P

QB = 128
KB = 32
PER_SPAN = 4
COMPACT = PER_SPAN * KB
CHUNKS = 8
F32 = jnp.float32
BF16 = jnp.bfloat16


def xor(value, bits):
    out = value
    for i in range(bits.bit_length()):
        if bits >> i & 1:
            out = out + (1 << i) - (2 << i) * lax.rem(value // (1 << i), 2)
    return out


def dot_nt(a, b):
    return lax.dot_general(a, b, (((1,), (1,)), ((), ())), preferred_element_type=F32)


def dot_tn(a, b):
    return lax.dot_general(a, b, (((0,), (0,)), ((), ())), preferred_element_type=F32)


def dot_nn(a, b):
    return lax.dot_general(a, b, (((1,), (0,)), ((), ())), preferred_element_type=F32)


def body(
    n, levels, heads, dh,
    picked_hbm, q_hbm, k_hbm, v_hbm, att_hbm, og_hbm, log_sum, x_hbm,
    dq_out, dk_out, dv_out, wg_out,
    picked, raw, q, k, v, att, og, x, xt, slot, slot_in, pick, ksend, kin, vsend, vin, dvsend, dvin, dksend, dkin,
    wts, part, got1, send2, got2, send3, got3,
    x_sem, picked_sem, raw_sem, slot_ss, slot_rs, k_ss, k_rs, v_ss, v_rs, dv_ss, dv_rs, dk_ss, dk_rs,
    s1_ss, s1_rs, s2_ss, s2_rs, s3_ss, s3_rs,
):
    me = lax.axis_index("kv")
    tok, cols = q.shape
    query_count = tok // QB
    span_blocks = tok // KB
    rows = slot.shape[0]
    scale = dh ** (-0.5)
    quarter = n // 4
    rb = wg_out.shape[0]
    order = list(reversed(range(levels)))

    def to(offset):
        return {"kv": lax.rem(me + offset + n, n)}

    def flipped(bits):
        low = lax.rem(me, 4)
        high = me // 4
        if bits == 1:
            return {"kv": me + 1 - 2 * lax.rem(me, 2)}
        if bits == 2:
            return {"kv": me + 2 - 4 * (low // 2)}
        return {"kv": xor(high, bits // 4) * 4 + low}

    def remote(src, dst, ss, rs, device):
        return pltpu.make_async_remote_copy(
            src_ref=src, dst_ref=dst, send_sem=ss, recv_sem=rs,
            device_id=device, device_id_type=pl.DeviceIdType.MESH,
        )

    load_picked = pltpu.make_async_copy(picked_hbm, picked, picked_sem)
    load_picked.start()
    loads = {}
    for i, (src, dst) in enumerate(
        ((k_hbm, k), (v_hbm, v), (q_hbm, q), (og_hbm, og), (att_hbm, att))
    ):
        loads[i] = (pltpu.make_async_copy(src, raw.at[i], raw_sem.at[i]), dst)
        loads[i][0].start()

    def settle(i):
        copy, dst = loads[i]
        copy.wait()
        for h in range(heads):
            dst[:, h * dh : (h + 1) * dh] = raw[i, :, h, :]

    load_x = pltpu.make_async_copy(x_hbm, x, x_sem)
    load_x.start()
    barrier = pltpu.get_barrier_semaphore()
    greeted = [to(1 << l) for l in range(levels)] + [to(-(1 << l)) for l in range(levels)]
    greeted += [flipped(1), flipped(2)] + [flipped(4 * b) for b in range(1, quarter)]
    for device in greeted:
        pl.semaphore_signal(
            barrier, inc=1, device_id=device, device_id_type=pl.DeviceIdType.MESH
        )

    row = lax.broadcasted_iota(jnp.int32, (rows, tok), 0)
    lane = lax.broadcasted_iota(jnp.int32, (rows, tok), 1)
    back = jnp.zeros((rows, tok), jnp.int32)
    for l in range(levels):
        back = jnp.where(row == l + 1, 1 << l, back)
    ids = jnp.where(row <= levels, (me - back) * span_blocks + lane // KB, -2)
    load_picked.wait()
    live = []
    for b in range(query_count):
        hit = jnp.zeros((rows, tok), jnp.int32)
        for s in range(picked.shape[1]):
            p = picked[b, s]
            hit = jnp.where(ids == jnp.where(p < 0, -(1 << 30), p), 1, hit)
        live.append(hit.astype(F32))
    need = functools.reduce(jnp.maximum, live)
    below = lax.broadcasted_iota(jnp.int32, (tok, tok), 0)
    above = lax.broadcasted_iota(jnp.int32, (tok, tok), 1)
    steps = jnp.where((below % KB == 0) & (below // KB < above // KB), 1.0, 0.0).astype(BF16)
    rank = dot_nn(need.astype(BF16), steps)
    slot[...] = jnp.where(need > 0, rank * KB + (lane % KB).astype(F32), -1.0)

    settle(0)
    settle(1)
    pl.semaphore_wait(barrier, len(greeted))

    def sends_up(l):
        return me + (1 << l) < n

    def sends_down(l):
        return me >= 1 << l

    slot_copies = {}
    for l in order:
        slot_copies[l] = remote(
            slot, slot_in.at[l], slot_ss.at[l], slot_rs.at[l], to(-(1 << l))
        )
        pl.when(sends_down(l))(slot_copies[l].start)

    def one_hot(row_values):
        sub = lax.broadcasted_iota(jnp.int32, (COMPACT, tok), 0).astype(F32)
        return jnp.where(sub == row_values, 1.0, 0.0).astype(BF16)

    head = [slice(h * dh, (h + 1) * dh) for h in range(heads)]
    k_copies, v_copies, dv_copies, dk_copies = {}, {}, {}, {}
    for l in order:
        k_copies[l] = remote(ksend.at[l], kin.at[l], k_ss.at[l], k_rs.at[l], to(1 << l))
        v_copies[l] = remote(vsend.at[l], vin.at[l], v_ss.at[l], v_rs.at[l], to(1 << l))
        dv_copies[l] = remote(
            dvsend.at[l], dvin.at[l], dv_ss.at[l], dv_rs.at[l], to(-(1 << l))
        )
        dk_copies[l] = remote(
            dksend.at[l], dkin.at[l], dk_ss.at[l], dk_rs.at[l], to(-(1 << l))
        )
    for l in order:

        @pl.when(sends_up(l))
        def _(l=l):
            slot_copies[l].wait_recv()
            chosen = one_hot(slot_in[l, l + 1 : l + 2, :])
            pick[l] = chosen
            ksend[l] = dot_nn(chosen, k[...]).astype(BF16)
            k_copies[l].start()

    for l in order:

        @pl.when(sends_up(l))
        def _(l=l):
            vsend[l] = dot_nn(pick[l], v[...]).astype(BF16)
            v_copies[l].start()

    for i in range(2, 5):
        settle(i)
    dots = []
    for c in head:
        column = jnp.sum(og[:, c].astype(F32) * att[:, c].astype(F32), axis=1, keepdims=True)
        dots.append(jnp.transpose(jnp.broadcast_to(column, (tok, 128)))[0:1, :])
    stored = [log_sum[h : h + 1, :] for h in range(heads)]

    def key_mask(chosen, r):
        pieces = []
        for m in live:
            column = dot_nt(chosen, m.astype(BF16))[:, r : r + 1]
            pieces.append(jnp.broadcast_to(column, (column.shape[0], QB)))
        return jnp.concatenate(pieces, axis=1) > 0

    own_mask = key_mask(jnp.where(below == above, 1.0, 0.0).astype(BF16), 0) & (below <= above)
    for h, c in enumerate(head):
        w = jnp.where(own_mask, jnp.exp(dot_nt(k[:, c], q[:, c]) * scale - stored[h]), 0.0)
        dv_out[:, c] = dot_nn(w.astype(BF16), og[:, c])
        g = (w * (dot_nt(v[:, c], og[:, c]) - dots[h])).astype(BF16)
        dk_out[:, c] = dot_nn(g, q[:, c])
        dq_out[:, c] = dot_tn(g, k[:, c])

    masks = {
        l: key_mask(one_hot(slot[l + 1 : l + 2, :]), l + 1) for l in order
    }
    load_x.wait()
    width = x.shape[1] // CHUNKS
    for i in range(CHUNKS):
        xt[i * width : (i + 1) * width, :] = jnp.transpose(x[:, i * width : (i + 1) * width])
    for l in range(levels):

        @pl.when(sends_down(l))
        def _(l=l):
            k_copies[l].wait_recv()
            for h, c in enumerate(head):
                w = jnp.where(
                    masks[l], jnp.exp(dot_nt(kin[l, :, c], q[:, c]) * scale - stored[h]), 0.0
                )
                wts[l, h] = w
                dvsend[l, :, c] = dot_nn(w.astype(BF16), og[:, c]).astype(BF16)
            dv_copies[l].start()

    for l in range(levels):

        @pl.when(sends_down(l))
        def _(l=l):
            v_copies[l].wait_recv()
            for h, c in enumerate(head):
                g = (wts[l, h] * (dot_nt(vin[l, :, c], og[:, c]) - dots[h])).astype(BF16)
                dksend[l, :, c] = (dot_nn(g, q[:, c]) * scale).astype(BF16)
                dq_out[:, c] += dot_tn(g, kin[l, :, c])
            dk_copies[l].start()

    dq_out[...] = dq_out[...] * scale

    for l in range(levels):

        @pl.when(sends_up(l))
        def _(l=l):
            dv_copies[l].wait_recv()
            dv_out[...] += dot_tn(pick[l], dvin[l])

    rounded = dv_out[...].astype(BF16)
    core = lax.rem(me, 2)
    up = lax.rem(me, 4) // 2
    high = me // 4
    far = list(reversed(range(quarter)))
    chunk = 2 * rb
    s1, s2, s3 = [], [], []

    def share(t, at):
        first = pl.multiple_of(at * chunk, chunk)
        w = dot_nn(xt[pl.ds(first, chunk), :], rounded)
        part[t] = w.reshape(2, rb, cols)
        copy = remote(
            part.at[t, 1 - core], got1.at[t], s1_ss.at[t], s1_rs.at[t], flipped(1)
        )
        copy.start()
        s1.append(copy)

    for t, b in enumerate(far):
        share(t, 2 * xor(high, b) + 1 - up)
    for t, b in enumerate(far):
        share(quarter + t, 2 * xor(high, b) + up)
        s1[t].wait_recv()
        send2[b] = (part[t, core] + got1[t]).astype(BF16)
        copy = remote(send2.at[b], got2.at[b], s2_ss.at[b], s2_rs.at[b], flipped(2))
        copy.start()
        s2.append(copy)
    for t, b in enumerate(far):
        s1[quarter + t].wait_recv()
        kept = part[quarter + t, core] + got1[quarter + t]
        s2[t].wait_recv()
        kept = kept + got2[b].astype(F32)
        if b == 0:
            wg_out[...] = kept
        else:
            send3[b] = kept.astype(BF16)
            copy = remote(send3.at[b], got3.at[b], s3_ss.at[b], s3_rs.at[b], flipped(4 * b))
            copy.start()
            s3.append(copy)

    dk_out[...] = dk_out[...] * scale
    for l in range(levels):

        @pl.when(sends_up(l))
        def _(l=l):
            dk_copies[l].wait_recv()
            dk_out[...] += dot_tn(pick[l], dkin[l])

    for b, copy in zip(reversed(range(1, quarter)), s3):
        copy.wait_recv()
        wg_out[...] += got3[b].astype(F32)
    for l in order:
        for copies in (slot_copies, dv_copies, dk_copies):
            pl.when(sends_down(l))(copies[l].wait_send)
        for copies in (k_copies, v_copies):
            pl.when(sends_up(l))(copies[l].wait_send)
    for copy in s1 + s2 + s3:
        copy.wait_send()


def per_device(queries, keys, values, attended, out_grad, log_sum, picked, layer_input):
    tok, heads, dh = queries.shape
    n = lax.axis_size("kv")
    levels = n.bit_length() - 1
    cols = heads * dh
    width = layer_input.shape[1]
    rb = width // n
    rows = (levels + 1 + 7) // 8 * 8
    hbm = pl.BlockSpec(memory_space=pltpu.HBM)
    vmem = pl.BlockSpec(memory_space=pltpu.VMEM)
    sems = pltpu.SemaphoreType.DMA
    level_buf = pltpu.VMEM((levels, COMPACT, cols), BF16)
    out = pl.pallas_call(
        functools.partial(body, n, levels, heads, dh),
        out_shape=[jax.ShapeDtypeStruct((tok, cols), F32)] * 3
        + [jax.ShapeDtypeStruct((rb, cols), F32)],
        in_specs=[hbm] * 6 + [vmem, hbm],
        out_specs=[vmem] * 4,
        scratch_shapes=[
            pltpu.SMEM(picked.shape, jnp.int32),
            pltpu.VMEM((5, tok, heads, dh), BF16),
        ]
        + [pltpu.VMEM((tok, cols), BF16)] * 5
        + [
            pltpu.VMEM((tok, width), BF16),
            pltpu.VMEM((width, tok), BF16),
            pltpu.VMEM((rows, tok), F32),
            pltpu.VMEM((levels, rows, tok), F32),
            pltpu.VMEM((levels, COMPACT, tok), BF16),
        ]
        + [level_buf] * 8
        + [
            pltpu.VMEM((levels, heads, COMPACT, tok), F32),
            pltpu.VMEM((n // 2, 2, rb, cols), F32),
            pltpu.VMEM((n // 2, rb, cols), F32),
            pltpu.VMEM((n // 4, rb, cols), BF16),
            pltpu.VMEM((n // 4, rb, cols), BF16),
            pltpu.VMEM((n // 4, rb, cols), BF16),
            pltpu.VMEM((n // 4, rb, cols), BF16),
            sems,
            sems,
            sems((5,)),
        ]
        + [sems((levels,))] * 10
        + [sems((n // 2,))] * 2
        + [sems((n // 4,))] * 4,
        compiler_params=pltpu.CompilerParams(
            collective_id=0, has_side_effects=True
        ),
    )(picked, queries, keys, values, attended, out_grad, log_sum.T, layer_input)
    grads = [g.reshape(tok, heads, dh) for g in out[:3]]
    return (*grads, out[3])


def solution(mesh):
    placed = (P("kv", "tp", None),) * 5 + (P("kv", "tp"), P("kv", None), P("kv", None))
    return jax.shard_map(
        per_device,
        mesh=mesh,
        in_specs=placed,
        out_specs=(P("kv", "tp", None), P("kv", "tp", None), P("kv", "tp", None), P("kv", "tp")),
        check_vma=False,
    )
```

```python
import functools

import jax
import jax.numpy as jnp
from jax import lax
from jax.experimental import pallas as pl
from jax.experimental.pallas import tpu as pltpu
from jax.sharding import PartitionSpec as P

QB = 128
KB = 32
PER_SPAN = 4
COMPACT = PER_SPAN * KB
CHUNKS = 8
F32 = jnp.float32
BF16 = jnp.bfloat16


def xor(value, bits):
    out = value
    for i in range(bits.bit_length()):
        if bits >> i & 1:
            out = out + (1 << i) - (2 << i) * lax.rem(value // (1 << i), 2)
    return out


def dot_nt(a, b):
    return lax.dot_general(a, b, (((1,), (1,)), ((), ())), preferred_element_type=F32)


def dot_tn(a, b):
    return lax.dot_general(a, b, (((0,), (0,)), ((), ())), preferred_element_type=F32)


def dot_nn(a, b):
    return lax.dot_general(a, b, (((1,), (0,)), ((), ())), preferred_element_type=F32)


def body(
    n, levels, heads, dh,
    picked_hbm, q_hbm, k_hbm, v_hbm, att_hbm, og_hbm, log_sum, x_hbm,
    dq_out, dk_out, dv_out, wg_out,
    picked, raw, q, k, v, att, og, x, xt, slot, slot_in, pick, ksend, kin, vsend, vin, dvsend, dvin, dksend, dkin,
    wts, part, got1, send2, got2, send3, got3,
    x_sem, picked_sem, raw_sem, slot_ss, slot_rs, k_ss, k_rs, v_ss, v_rs, dv_ss, dv_rs, dk_ss, dk_rs,
    s1_ss, s1_rs, s2_ss, s2_rs, s3_ss, s3_rs,
):
    me = lax.axis_index("kv")
    tok, cols = q.shape
    query_count = tok // QB
    span_blocks = tok // KB
    rows = slot.shape[0]
    scale = dh ** (-0.5)
    quarter = n // 4
    rb = wg_out.shape[0]
    order = list(reversed(range(levels)))

    def to(offset):
        return {"kv": lax.rem(me + offset + n, n)}

    def flipped(bits):
        low = lax.rem(me, 4)
        high = me // 4
        if bits == 1:
            return {"kv": me + 1 - 2 * lax.rem(me, 2)}
        if bits == 2:
            return {"kv": me + 2 - 4 * (low // 2)}
        return {"kv": xor(high, bits // 4) * 4 + low}

    def remote(src, dst, ss, rs, device):
        return pltpu.make_async_remote_copy(
            src_ref=src, dst_ref=dst, send_sem=ss, recv_sem=rs,
            device_id=device, device_id_type=pl.DeviceIdType.MESH,
        )

    load_picked = pltpu.make_async_copy(picked_hbm, picked, picked_sem)
    load_picked.start()
    loads = {}
    for i, (src, dst) in enumerate(
        ((k_hbm, k), (v_hbm, v), (q_hbm, q), (og_hbm, og), (att_hbm, att))
    ):
        loads[i] = (pltpu.make_async_copy(src, raw.at[i], raw_sem.at[i]), dst)
        loads[i][0].start()

    def settle(i):
        copy, dst = loads[i]
        copy.wait()
        for h in range(heads):
            dst[:, h * dh : (h + 1) * dh] = raw[i, :, h, :]

    load_x = pltpu.make_async_copy(x_hbm, x, x_sem)
    load_x.start()
    barrier = pltpu.get_barrier_semaphore()
    greeted = [to(1 << l) for l in range(levels)] + [to(-(1 << l)) for l in range(levels)]
    greeted += [flipped(1), flipped(2)] + [flipped(4 * b) for b in range(1, quarter)]
    for device in greeted:
        pl.semaphore_signal(
            barrier, inc=1, device_id=device, device_id_type=pl.DeviceIdType.MESH
        )

    row = lax.broadcasted_iota(jnp.int32, (rows, tok), 0)
    lane = lax.broadcasted_iota(jnp.int32, (rows, tok), 1)
    back = jnp.zeros((rows, tok), jnp.int32)
    for l in range(levels):
        back = jnp.where(row == l + 1, 1 << l, back)
    ids = jnp.where(row <= levels, (me - back) * span_blocks + lane // KB, -2)
    load_picked.wait()
    live = []
    for b in range(query_count):
        hit = jnp.zeros((rows, tok), jnp.int32)
        for s in range(picked.shape[1]):
            p = picked[b, s]
            hit = jnp.where(ids == jnp.where(p < 0, -(1 << 30), p), 1, hit)
        live.append(hit.astype(F32))
    need = functools.reduce(jnp.maximum, live)
    below = lax.broadcasted_iota(jnp.int32, (tok, tok), 0)
    above = lax.broadcasted_iota(jnp.int32, (tok, tok), 1)
    steps = jnp.where((below % KB == 0) & (below // KB < above // KB), 1.0, 0.0).astype(BF16)
    rank = dot_nn(need.astype(BF16), steps)
    slot[...] = jnp.where(need > 0, rank * KB + (lane % KB).astype(F32), -1.0)

    settle(0)
    settle(1)
    pl.semaphore_wait(barrier, len(greeted))

    def sends_up(l):
        return me + (1 << l) < n

    def sends_down(l):
        return me >= 1 << l

    slot_copies = {}
    for l in order:
        slot_copies[l] = remote(
            slot, slot_in.at[l], slot_ss.at[l], slot_rs.at[l], to(-(1 << l))
        )
        pl.when(sends_down(l))(slot_copies[l].start)

    def one_hot(row_values):
        sub = lax.broadcasted_iota(jnp.int32, (COMPACT, tok), 0).astype(F32)
        return jnp.where(sub == row_values, 1.0, 0.0).astype(BF16)

    head = [slice(h * dh, (h + 1) * dh) for h in range(heads)]
    k_copies, v_copies, dv_copies, dk_copies = {}, {}, {}, {}
    for l in order:
        k_copies[l] = remote(ksend.at[l], kin.at[l], k_ss.at[l], k_rs.at[l], to(1 << l))
        v_copies[l] = remote(vsend.at[l], vin.at[l], v_ss.at[l], v_rs.at[l], to(1 << l))
        dv_copies[l] = remote(
            dvsend.at[l], dvin.at[l], dv_ss.at[l], dv_rs.at[l], to(-(1 << l))
        )
        dk_copies[l] = remote(
            dksend.at[l], dkin.at[l], dk_ss.at[l], dk_rs.at[l], to(-(1 << l))
        )
    for l in order:

        @pl.when(sends_up(l))
        def _(l=l):
            slot_copies[l].wait_recv()
            chosen = one_hot(slot_in[l, l + 1 : l + 2, :])
            pick[l] = chosen
            ksend[l] = dot_nn(chosen, k[...]).astype(BF16)
            k_copies[l].start()

    for l in order:

        @pl.when(sends_up(l))
        def _(l=l):
            vsend[l] = dot_nn(pick[l], v[...]).astype(BF16)
            v_copies[l].start()

    for i in range(2, 5):
        settle(i)
    dots = []
    for c in head:
        column = jnp.sum(og[:, c].astype(F32) * att[:, c].astype(F32), axis=1, keepdims=True)
        dots.append(jnp.transpose(jnp.broadcast_to(column, (tok, 128)))[0:1, :])
    stored = [log_sum[h : h + 1, :] for h in range(heads)]

    def key_mask(chosen, r):
        pieces = []
        for m in live:
            column = dot_nt(chosen, m.astype(BF16))[:, r : r + 1]
            pieces.append(jnp.broadcast_to(column, (column.shape[0], QB)))
        return jnp.concatenate(pieces, axis=1) > 0

    own_mask = key_mask(jnp.where(below == above, 1.0, 0.0).astype(BF16), 0) & (below <= above)
    for h, c in enumerate(head):
        w = jnp.where(own_mask, jnp.exp(dot_nt(k[:, c], q[:, c]) * scale - stored[h]), 0.0)
        dv_out[:, c] = dot_nn(w.astype(BF16), og[:, c])
        g = (w * (dot_nt(v[:, c], og[:, c]) - dots[h])).astype(BF16)
        dk_out[:, c] = dot_nn(g, q[:, c])
        dq_out[:, c] = dot_tn(g, k[:, c])

    masks = {
        l: key_mask(one_hot(slot[l + 1 : l + 2, :]), l + 1) for l in order
    }
    load_x.wait()
    width = x.shape[1] // CHUNKS
    for i in range(CHUNKS):
        xt[i * width : (i + 1) * width, :] = jnp.transpose(x[:, i * width : (i + 1) * width])
    for l in range(levels):

        @pl.when(sends_down(l))
        def _(l=l):
            k_copies[l].wait_recv()
            for h, c in enumerate(head):
                w = jnp.where(
                    masks[l], jnp.exp(dot_nt(kin[l, :, c], q[:, c]) * scale - stored[h]), 0.0
                )
                wts[l, h] = w
                dvsend[l, :, c] = dot_nn(w.astype(BF16), og[:, c]).astype(BF16)
            dv_copies[l].start()

    for l in range(levels):

        @pl.when(sends_down(l))
        def _(l=l):
            v_copies[l].wait_recv()
            for h, c in enumerate(head):
                g = (wts[l, h] * (dot_nt(vin[l, :, c], og[:, c]) - dots[h])).astype(BF16)
                dksend[l, :, c] = (dot_nn(g, q[:, c]) * scale).astype(BF16)
                dq_out[:, c] += dot_tn(g, kin[l, :, c])
            dk_copies[l].start()

    dq_out[...] = dq_out[...] * scale

    for l in range(levels):

        @pl.when(sends_up(l))
        def _(l=l):
            dv_copies[l].wait_recv()
            dv_out[...] += dot_tn(pick[l], dvin[l])

    rounded = dv_out[...].astype(BF16)
    core = lax.rem(me, 2)
    up = lax.rem(me, 4) // 2
    high = me // 4
    far = list(reversed(range(quarter)))
    chunk = 2 * rb
    s1, s2, s3 = [], [], []

    def share(t, at):
        first = pl.multiple_of(at * chunk, chunk)
        w = dot_nn(xt[pl.ds(first, chunk), :], rounded)
        part[t] = w.reshape(2, rb, cols)
        copy = remote(
            part.at[t, 1 - core], got1.at[t], s1_ss.at[t], s1_rs.at[t], flipped(1)
        )
        copy.start()
        s1.append(copy)

    for t, b in enumerate(far):
        share(t, 2 * xor(high, b) + 1 - up)
    for t, b in enumerate(far):
        share(quarter + t, 2 * xor(high, b) + up)
        s1[t].wait_recv()
        send2[b] = (part[t, core] + got1[t]).astype(BF16)
        copy = remote(send2.at[b], got2.at[b], s2_ss.at[b], s2_rs.at[b], flipped(2))
        copy.start()
        s2.append(copy)
    for t, b in enumerate(far):
        s1[quarter + t].wait_recv()
        kept = part[quarter + t, core] + got1[quarter + t]
        s2[t].wait_recv()
        kept = kept + got2[b].astype(F32)
        if b == 0:
            wg_out[...] = kept
        else:
            send3[b] = kept.astype(BF16)
            copy = remote(send3.at[b], got3.at[b], s3_ss.at[b], s3_rs.at[b], flipped(4 * b))
            copy.start()
            s3.append(copy)

    dk_out[...] = dk_out[...] * scale
    for l in range(levels):

        @pl.when(sends_up(l))
        def _(l=l):
            dk_copies[l].wait_recv()
            dk_out[...] += dot_tn(pick[l], dkin[l])

    for b, copy in zip(reversed(range(1, quarter)), s3):
        copy.wait_recv()
        wg_out[...] += got3[b].astype(F32)
    for l in order:
        for copies in (slot_copies, dv_copies, dk_copies):
            pl.when(sends_down(l))(copies[l].wait_send)
        for copies in (k_copies, v_copies):
            pl.when(sends_up(l))(copies[l].wait_send)
    for copy in s1 + s2 + s3:
        copy.wait_send()


def finish(dq, dk, dv, wg, dq_out, dk_out, dv_out, wg_out):
    heads, dh = dq_out.shape[1:]
    for src, dst in ((dq, dq_out), (dk, dk_out), (dv, dv_out)):
        for h in range(heads):
            dst[:, h, :] = src[:, h * dh : (h + 1) * dh]
    wg_out[...] = wg[...]


def per_device(queries, keys, values, attended, out_grad, log_sum, picked, layer_input):
    tok, heads, dh = queries.shape
    n = lax.axis_size("kv")
    levels = n.bit_length() - 1
    cols = heads * dh
    width = layer_input.shape[1]
    rb = width // n
    rows = (levels + 1 + 7) // 8 * 8
    hbm = pl.BlockSpec(memory_space=pltpu.HBM)
    vmem = pl.BlockSpec(memory_space=pltpu.VMEM)
    sems = pltpu.SemaphoreType.DMA
    level_buf = pltpu.VMEM((levels, COMPACT, cols), BF16)
    out = pl.pallas_call(
        functools.partial(body, n, levels, heads, dh),
        out_shape=[jax.ShapeDtypeStruct((tok, cols), F32)] * 3
        + [jax.ShapeDtypeStruct((rb, cols), F32)],
        in_specs=[hbm] * 6 + [vmem, hbm],
        out_specs=[vmem] * 4,
        scratch_shapes=[
            pltpu.SMEM(picked.shape, jnp.int32),
            pltpu.VMEM((5, tok, heads, dh), BF16),
        ]
        + [pltpu.VMEM((tok, cols), BF16)] * 5
        + [
            pltpu.VMEM((tok, width), BF16),
            pltpu.VMEM((width, tok), BF16),
            pltpu.VMEM((rows, tok), F32),
            pltpu.VMEM((levels, rows, tok), F32),
            pltpu.VMEM((levels, COMPACT, tok), BF16),
        ]
        + [level_buf] * 8
        + [
            pltpu.VMEM((levels, heads, COMPACT, tok), F32),
            pltpu.VMEM((n // 2, 2, rb, cols), F32),
            pltpu.VMEM((n // 2, rb, cols), F32),
            pltpu.VMEM((n // 4, rb, cols), BF16),
            pltpu.VMEM((n // 4, rb, cols), BF16),
            pltpu.VMEM((n // 4, rb, cols), BF16),
            pltpu.VMEM((n // 4, rb, cols), BF16),
            sems,
            sems,
            sems((5,)),
        ]
        + [sems((levels,))] * 10
        + [sems((n // 2,))] * 2
        + [sems((n // 4,))] * 4,
        compiler_params=pltpu.CompilerParams(
            collective_id=0, has_side_effects=True
        ),
    )(picked, queries, keys, values, attended, out_grad, log_sum.T, layer_input)
    return pl.pallas_call(
        finish,
        out_shape=[jax.ShapeDtypeStruct((tok, heads, dh), F32)] * 3
        + [jax.ShapeDtypeStruct((rb, cols), F32)],
        in_specs=[vmem] * 4,
        out_specs=[vmem] * 4,
    )(*out)


def solution(mesh):
    placed = (P("kv", "tp", None),) * 5 + (P("kv", "tp"), P("kv", None), P("kv", None))
    return jax.shard_map(
        per_device,
        mesh=mesh,
        in_specs=placed,
        out_specs=(P("kv", "tp", None), P("kv", "tp", None), P("kv", "tp", None), P("kv", "tp")),
        check_vma=False,
    )
```
